32 devices in a mesh: kv: 8 (over z, core), tp: 4 (over y, x).
Axes of the slice: x: 2, y: 2, z: 4, core: 2. Of those that a mesh axis runs over, the one named last changes fastest.
Arguments:
- tokens: bfloat16 [24, 4096], P(None, 'kv'), may hold values from -24 to 24
- attention_norm_gain: float32 [4096], replicated, may hold values from 0.1 to 1.9
- query_weight: bfloat16 [4096, 2048], P('kv', 'tp'), may hold values from -0.09375 to 0.09375
- key_weight: bfloat16 [4096, 2048], P('kv', 'tp'), may hold values from -0.09375 to 0.09375
- value_weight: bfloat16 [4096, 4096], P('kv', 'tp'), may hold values from -0.09375 to 0.09375
- output_gate_weight: bfloat16 [4096, 4096], P('kv', 'tp'), may hold values from -0.09375 to 0.09375
- lowrank_weight: bfloat16 [4096, 16], replicated, may hold values from -0.09375 to 0.09375
- decay_weight: bfloat16 [16, 2048], replicated, may hold values from -1.5 to 1.5
- decay_preact_bias: float32 [2048], replicated, may hold values from -1 to 20
- head_norm_gain: float32 [256], replicated, may hold values from 0.1 to 1.9
- output_weight: bfloat16 [4096, 4096], P('tp', 'kv'), may hold values from -0.125 to 0.125
- feedforward_norm_gain: float32 [4096], replicated, may hold values from 0.1 to 1.9
- feedforward_gate_weight: bfloat16 [4096, 10240], P('kv', 'tp'), may hold values from -0.09375 to 0.09375
- feedforward_up_weight: bfloat16 [4096, 10240], P('kv', 'tp'), may hold values from -0.09375 to 0.09375
- feedforward_down_weight: bfloat16 [10240, 4096], P('tp', 'kv'), may hold values from -0.078125 to 0.078125
- past_key_cache: bfloat16 [24, 1536, 2048], P(None, 'kv', 'tp'), may hold values from -6 to 6
- past_value_cache: bfloat16 [24, 1536, 4096], P(None, 'kv', 'tp'), may hold values from -6 to 6
- past_lowrank_cache: bfloat16 [24, 16, 1536], P(None, None, 'kv'), may hold values from -8 to 8
- head_extra_decay: float32 [24, 16, 1536], P(None, 'tp', 'kv'), may hold values from -0.7 to 0
- lengths: int32 [24], replicated, may hold values from 1 to 1536, 10368 in all
Outputs:
- output: bfloat16 [24, 4096], P(None, 'kv')
The draws below stay inside these ranges and needn't reach their ends.
All inputs are finite; a program needn't handle non-finite values.
Results may differ from the reference program's by a relative error of at most 0.0085.
Values may be sent and summed in bfloat16 or wider, within the bound.
A program may use at most 128 MiB of HBM per device.

```python
import math
import jax
import jax.numpy as jnp
import numpy as np
from jax import lax

D = 4096
HEADS = 16
KEY_CHANNELS = 128
DV = 256
RANK = 16
FF = 10240
SEQS = 24
POS_DEV = 192
LENGTH = 1536
KEYDIM = 2048
VALDIM = 4096


def draw_tokens(key, part):
    key_base, key_rows = jax.random.split(jax.random.fold_in(key, 11))
    columns = jnp.arange(D, dtype=jnp.float32) / D
    standard = jax.random.normal(key_base, (SEQS, D), jnp.float32)
    col_scale = 0.32 * 10.0 ** columns
    row_scale = jnp.exp(jax.random.uniform(key_rows, (SEQS, 1), jnp.float32, -1.15, 1.15))
    return jnp.clip(standard * col_scale[None, :] * row_scale, -24.0, 24.0).astype(jnp.bfloat16)


def draw_decay_preact_bias(key, part):
    key_pick, key_fast, key_slow = jax.random.split(jax.random.fold_in(key, 23), 3)
    order = jax.random.permutation(key_pick, HEADS)
    fast_value = jax.random.uniform(key_fast, (HEADS, KEY_CHANNELS), jnp.float32, -1.0, 0.5)
    fast_head = order < HEADS // 2
    slow_value = jnp.log(LENGTH * 1.0) + jax.random.uniform(key_slow, (HEADS, KEY_CHANNELS), jnp.float32, 1.0, 3.0)
    return jnp.where(fast_head[:, None], fast_value, slow_value).reshape(HEADS * KEY_CHANNELS).astype(jnp.float32)


def draw_past_lowrank_cache(key, part):
    key_value, key_scale = jax.random.split(jax.random.fold_in(key, 37))
    groups = LENGTH // POS_DEV
    standard = jax.random.normal(key_value, (SEQS, RANK, groups, POS_DEV), jnp.float32)
    group_scale = jnp.exp(jax.random.uniform(key_scale, (SEQS, 1, groups, 1), jnp.float32, -0.7, 0.7))
    return jnp.clip((standard * group_scale).reshape(SEQS, RANK, LENGTH), -8.0, 8.0).astype(jnp.bfloat16)


def draw_head_extra_decay(key, part):
    key_where, key_depth = jax.random.split(jax.random.fold_in(key, 41))
    array_shape = (SEQS, HEADS, LENGTH)
    struck = jax.random.uniform(key_where, array_shape, jnp.float32) < 4.0 / LENGTH
    kept = jax.random.uniform(key_depth, array_shape, jnp.float32, 0.5, 0.8)
    return jnp.where(struck, jnp.log(kept), 0.0).astype(jnp.float32)


def raised(entries, own_key, source, target, blocks, factor):
    def block_of(position):
        return (jnp.arange(entries.shape[position]) // (entries.shape[position] // blocks)).reshape((-1,) + (1,) * (entries.ndim - 1 - position))

    first = jax.random.permutation(own_key, blocks)[block_of(target)]
    second = (block_of(target) + blocks // 2) % blocks
    return jnp.where((block_of(source) == first) | (block_of(source) == second), factor * entries, entries)


def block_levels(stream_key, dims, cuts, low, high):
    gain, own = 1.0, jax.random.fold_in(stream_key, 6)
    for position, shards_of in cuts:
        draws = jnp.exp(jax.random.uniform(jax.random.fold_in(own, position), (shards_of,), jnp.float32, low / len(cuts), high / len(cuts)))
        gain = gain * jnp.repeat(draws, dims[position] // shards_of).reshape([-1 if axis == position else 1 for axis in range(len(dims))])
    return gain


def split_up(number_of, total, reach, skew):
    loads = [(1 << 20) // math.isqrt(standing ** skew) + 1 for standing in range(2, number_of + 1)]
    spare, given = total - reach - (number_of - 1), [1] * (number_of - 1)
    while spare > 0:
        movable = [i for i in range(number_of - 1) if given[i] < reach]
        whole, remaining = sum([loads[i] for i in movable]), spare
        for i in movable:
            more = min(reach - given[i], max(1, remaining * loads[i] // whole), spare)
            given[i] = given[i] + more
            spare = spare - more
    return np.array([reach] + given)


def uneven_parts(rng, number_of, total, reach, lean):
    if number_of == 2:
        one = jax.random.randint(rng, (), max(1, total - reach), min(reach, total - 1) + 1)
        return jnp.stack([one, total - one])
    sizes = jnp.asarray(split_up(number_of, total, reach, lean), jnp.int32)
    couples = (number_of - 1) // 2
    source_of, taker = sizes[1:1 + 2 * couples:2], sizes[2:2 + 2 * couples:2]
    room = jnp.minimum(source_of - 1, reach - taker)
    moved = jax.random.randint(jax.random.fold_in(rng, 1), (couples,), 0, 1 << 20) % (room + 1)
    sizes = sizes.at[1:1 + 2 * couples:2].set(source_of - moved).at[2:2 + 2 * couples:2].set(taker + moved)
    return sizes[jax.random.permutation(jax.random.fold_in(rng, 2), number_of)]


def scatter_about(rng, extent, width, reach, cuts=(), kind=jnp.bfloat16):
    level = block_levels(rng, extent, cuts, -0.22, 0.18) if cuts else 1.0
    array = jax.random.normal(rng, extent, jnp.float32) * width * level
    return jnp.minimum(jnp.maximum(array, -reach), reach).astype(kind)


def bell_draw_with(rng, extent, deviation, reach, shards, heavy, kind=jnp.bfloat16):
    values = deviation * jax.random.normal(rng, extent, jnp.float32)
    if shards:
        values = values * block_levels(rng, extent, shards, -0.22, 0.18)
    return jnp.clip(raised(values, jax.random.fold_in(rng, 3), *heavy), -reach, reach).astype(kind)


def setup_inputs(seed: int = 0) -> dict:
    arg_keys = jax.random.split(jax.random.key(seed), 21)
    return {
        "tokens": draw_tokens(jax.random.fold_in(arg_keys[20], 71), 0),
        "attention_norm_gain": jnp.clip(1.0 + 0.18 * jax.random.normal(arg_keys[1], (D,), jnp.float32), 0.1, 1.9),
        "query_weight": scatter_about(arg_keys[2], (D, KEYDIM), D ** -0.5, 0.09375, ((0, 8), (1, 4))),
        "key_weight": scatter_about(arg_keys[3], (D, KEYDIM), D ** -0.5, 0.09375, ((0, 8), (1, 4))),
        "value_weight": scatter_about(arg_keys[4], (D, VALDIM), D ** -0.5, 0.09375, ((0, 8), (1, 4))),
        "output_gate_weight": scatter_about(arg_keys[5], (D, VALDIM), D ** -0.5, 0.09375, ((0, 8), (1, 4))),
        "lowrank_weight": scatter_about(arg_keys[6], (D, RANK), D ** -0.5, 0.09375),
        "decay_weight": scatter_about(arg_keys[7], (RANK, KEYDIM), RANK ** -0.5, 1.5),
        "decay_preact_bias": draw_decay_preact_bias(jax.random.fold_in(arg_keys[20], 71), 0),
        "head_norm_gain": jnp.clip(1.0 + 0.18 * jax.random.normal(arg_keys[9], (DV,), jnp.float32), 0.1, 1.9),
        "output_weight": bell_draw_with(arg_keys[10], (VALDIM, D), VALDIM ** -0.5, 0.125, ((0, 4), (1, 8)), (0, 1, 8, 2.0)),
        "feedforward_norm_gain": jnp.clip(1.0 + 0.18 * jax.random.normal(arg_keys[11], (D,), jnp.float32), 0.1, 1.9),
        "feedforward_gate_weight": scatter_about(arg_keys[12], (D, FF), D ** -0.5, 0.09375, ((0, 8), (1, 4))),
        "feedforward_up_weight": scatter_about(arg_keys[13], (D, FF), D ** -0.5, 0.09375, ((0, 8), (1, 4))),
        "feedforward_down_weight": bell_draw_with(arg_keys[14], (FF, D), FF ** -0.5, 0.078125, ((0, 4), (1, 8)), (0, 1, 8, 2.0)),
        "past_key_cache": scatter_about(arg_keys[15], (SEQS, LENGTH, KEYDIM), 1.0, 6.0, ((1, 8), (2, 4))),
        "past_value_cache": scatter_about(arg_keys[16], (SEQS, LENGTH, VALDIM), 1.0, 6.0, ((1, 8), (2, 4))),
        "past_lowrank_cache": draw_past_lowrank_cache(jax.random.fold_in(arg_keys[20], 71), 0),
        "head_extra_decay": draw_head_extra_decay(jax.random.fold_in(arg_keys[20], 71), 0),
        "lengths": uneven_parts(arg_keys[19], SEQS, (SEQS + 3) * LENGTH // 4, LENGTH, 2).astype(jnp.int32),
    }


NORM_EPSILON = 1e-06

def product(operand, weights):
    return jnp.dot(operand, weights, preferred_element_type=jnp.float32)

def reference(tokens, attention_norm_gain, query_weight, key_weight, value_weight, output_gate_weight, lowrank_weight, decay_weight, decay_preact_bias, head_norm_gain, output_weight, feedforward_norm_gain, feedforward_gate_weight, feedforward_up_weight, feedforward_down_weight, past_key_cache, past_value_cache, past_lowrank_cache, head_extra_decay, lengths):
    sequences = tokens.shape[0]
    rows_float = tokens.astype(jnp.float32)
    inv_rms = lax.rsqrt(lax.optimization_barrier(jnp.mean(rows_float * rows_float, axis=1, keepdims=True)) + NORM_EPSILON)
    scaled = (rows_float * attention_norm_gain).astype(jnp.bfloat16)
    query_vector = (inv_rms * product(scaled, query_weight)).astype(jnp.bfloat16)
    fresh_key = (inv_rms * product(scaled, key_weight)).astype(jnp.bfloat16)
    fresh_value = (inv_rms * product(scaled, value_weight)).astype(jnp.bfloat16)
    outgate = (inv_rms * product(scaled, output_gate_weight)).astype(jnp.bfloat16)
    lowrank = (inv_rms * product(scaled, lowrank_weight)).astype(jnp.bfloat16)
    fresh_gate_value = jax.nn.log_sigmoid(product(lowrank, decay_weight) + decay_preact_bias) / 16.0

    def single_sequence(layer_inputs):
        key_matrix, value_matrix, lowrank_inputs, extra_decays, valid_length, query_single, key_vector, value_vector, gate_vector = layer_inputs
        gate_preactivation = jnp.dot(lowrank_inputs.T, decay_weight, preferred_element_type=jnp.float32) + decay_preact_bias
        decay_gates = jax.nn.log_sigmoid(gate_preactivation) / 16.0 + jnp.repeat(extra_decays.T, KEY_CHANNELS, axis=1)
        is_live = jnp.arange(key_matrix.shape[0], dtype=jnp.int32) < valid_length
        decay_gates = jnp.where(is_live[:, None], decay_gates, 0.0)
        suffix = jnp.cumsum(decay_gates[::-1], axis=0)[::-1]
        exclusive = jnp.concatenate([suffix[1:], jnp.zeros((1, suffix.shape[1]), jnp.float32)], axis=0)
        weighting = jnp.exp(exclusive + gate_vector[None, :])
        query_scaled = query_single.astype(jnp.float32) * KEY_CHANNELS ** (-0.5)
        products = key_matrix.astype(jnp.float32) * weighting * query_scaled[None, :]
        scores = lax.optimization_barrier(jnp.sum(products.reshape(key_matrix.shape[0], HEADS, KEY_CHANNELS), axis=2))
        scores = jnp.where(is_live[:, None], scores, 0.0).astype(jnp.bfloat16)
        summed = jnp.einsum('lh,lhv->hv', scores.astype(jnp.float32), value_matrix.astype(jnp.float32).reshape(key_matrix.shape[0], HEADS, DV), precision=lax.Precision.HIGHEST)
        own_score = lax.optimization_barrier(jnp.sum((query_scaled * key_vector.astype(jnp.float32)).reshape(HEADS, KEY_CHANNELS), axis=1))
        return summed + own_score[:, None] * value_vector.astype(jnp.float32).reshape(HEADS, DV)
    mixer_output = lax.map(single_sequence, (past_key_cache, past_value_cache, past_lowrank_cache, head_extra_decay, lengths, query_vector, fresh_key, fresh_value, fresh_gate_value))
    mean_sq = lax.optimization_barrier(jnp.mean(mixer_output * mixer_output, axis=2, keepdims=True))
    gate_act = jax.nn.silu(outgate.astype(jnp.float32).reshape(sequences, HEADS, DV))
    gated = (mixer_output * lax.rsqrt(mean_sq + NORM_EPSILON) * head_norm_gain * gate_act).astype(jnp.bfloat16)
    residual = rows_float + product(gated.reshape(sequences, HEADS * DV), output_weight)
    inv_two = lax.rsqrt(lax.optimization_barrier(jnp.mean(residual * residual, axis=1, keepdims=True)) + NORM_EPSILON)
    scaled_two = (residual * feedforward_norm_gain).astype(jnp.bfloat16)
    hidden = (jax.nn.silu(inv_two * product(scaled_two, feedforward_gate_weight)) * (inv_two * product(scaled_two, feedforward_up_weight))).astype(jnp.bfloat16)
    return (residual + product(hidden, feedforward_down_weight)).astype(jnp.bfloat16)
```

```python
import functools

import jax
import jax.numpy as jnp
from jax import lax
from jax.experimental import pallas as pl
from jax.experimental.pallas import tpu as pltpu
from jax.sharding import PartitionSpec as P

NORM_EPSILON = 1e-06
LANES = 128
CHUNK = 512
F32 = jnp.float32
BF16 = jnp.bfloat16


def dot(a, b):
    return jnp.dot(a, b, preferred_element_type=F32)


def log_sigmoid(v):
    return jnp.minimum(v, 0.0) - jnp.log(1.0 + jnp.exp(-jnp.abs(v)))


def remote(src, dst, send_sem, recv_sem, axis, dest):
    return pltpu.make_async_remote_copy(
        src_ref=src,
        dst_ref=dst,
        send_sem=send_sem,
        recv_sem=recv_sem,
        device_id={axis: dest},
        device_id_type=pl.DeviceIdType.MESH,
    )


class Exchange:
    def __init__(self, axis, size, out, slots, send_sem, recv_sem, same=False):
        self.axis, self.size, self.out, self.slots = axis, size, out, slots
        self.send_sem, self.recv_sem, self.same = send_sem, recv_sem, same
        self.me = lax.axis_index(axis)

    def source(self, dest):
        return self.out if self.same else self.out.at[dest]

    def to(self, dest):
        return remote(
            self.source(dest), self.slots.at[self.me], self.send_sem.at[dest],
            self.recv_sem.at[self.me], self.axis, dest,
        )

    def start(self):
        for k in range(1, self.size):
            self.to(lax.rem(self.me + k, self.size)).start()

    def arrived(self, origin):
        remote(
            self.source(origin), self.slots.at[origin], self.send_sem.at[origin],
            self.recv_sem.at[origin], self.axis, origin,
        ).wait_recv()

    def wait_recv(self):
        for k in range(1, self.size):
            self.arrived(lax.rem(self.me + k, self.size))

    def wait_send(self):
        for k in range(1, self.size):
            self.to(lax.rem(self.me + k, self.size)).wait_send()


def layer(
    n, m, spd,
    tokens_h, gain1_h, wq_h, wk_h, wv_h, wo_h, low_h, dw_h, bias_h, hgain_h, wout_h,
    gain2_h, wg_h, wu_h, wd_h, key_h, val_h, lr_h, ext_h, len_ref,
    out_ref,
    tokens, gain1, wq, wk, wv, wo, low, dw, bias, hgain, wout, gain2, wg, wu, wd,
    key, val, lr, ext,
    tri, tri_t, efac, a_full, a_send, a_recv, t_send, t_recv, q_send, q_recv,
    p_send, p_recv, g_own, g_recv, g_full, o_own, o_recv, s_own, s_recv,
    e_send, e_recv, h_own, h_recv, f_own, f_recv,
    in_sem, key_sem, val_sem, kv_ss, kv_rs, tp_ss, tp_rs,
):
    me = lax.axis_index("kv")
    mt = lax.axis_index("tp")
    seqs, width = tokens.shape
    chans, vals = wq.shape[1], wv.shape[1]
    heads, positions = ext.shape[1], ext.shape[2]
    kc, dv = chans // heads, vals // heads
    rank = low.shape[1]
    hidden = wg.shape[1]
    hw = e_send.shape[2]
    model = width * n

    def rows_of(ref, start, size):
        return ref.at[pl.ds(pl.multiple_of(start, size), size)]

    def cols_of(ref, start, size):
        return ref.at[:, pl.ds(pl.multiple_of(start, size), size)]

    sources = [
        (tokens_h, tokens),
        (cols_of(gain1_h, me * width, width), gain1),
        (wq_h, wq), (wk_h, wk), (wv_h, wv), (wo_h, wo),
        (rows_of(low_h, me * width, width), low),
        (cols_of(dw_h, mt * chans, chans), dw),
        (cols_of(bias_h, mt * chans, chans), bias),
        (lr_h, lr), (ext_h, ext),
    ]
    later = [
        (hgain_h, hgain), (wout_h, wout),
        (cols_of(gain2_h, me * width, width), gain2),
        (wg_h, wg), (wu_h, wu), (wd_h, wd),
    ]
    fetch = [pltpu.make_async_copy(a, b, in_sem.at[i]) for i, (a, b) in enumerate(sources + later)]
    for c in fetch[:len(sources)]:
        c.start()

    def key_copy(s):
        return pltpu.make_async_copy(key_h.at[s], key.at[s], key_sem.at[s])

    def val_copy(s):
        return pltpu.make_async_copy(val_h.at[s], val.at[s], val_sem.at[s])

    pl.loop(0, seqs)(lambda s: key_copy(s).start())
    pl.loop(0, seqs)(lambda s: val_copy(s).start())
    for c in fetch[len(sources):]:
        c.start()

    barrier = pltpu.get_barrier_semaphore()
    for axis, size, own in (("kv", n, me), ("tp", m, mt)):
        for k in range(1, size):
            pl.semaphore_signal(
                barrier, inc=1, device_id={axis: lax.rem(own + k, size)},
                device_id_type=pl.DeviceIdType.MESH,
            )

    def kv_exchange(i, out, slots, same=False):
        return Exchange("kv", n, out, slots, kv_ss.at[i], kv_rs.at[i], same)

    def tp_exchange(i, out, slots):
        return Exchange("tp", m, out, slots, tp_ss.at[i], tp_rs.at[i], True)

    ax = kv_exchange(0, a_send, a_recv)
    tx = kv_exchange(1, t_send, t_recv)
    qx = kv_exchange(2, q_send, q_recv)
    px = kv_exchange(3, p_send, p_recv)
    gx = kv_exchange(4, g_own, g_recv, True)
    sx = kv_exchange(5, s_own, s_recv, True)
    ex = kv_exchange(6, e_send, e_recv)
    hx = kv_exchange(7, h_own, h_recv, True)
    ox = tp_exchange(0, o_own, o_recv)
    fx = tp_exchange(1, f_own, f_recv)

    row = lax.broadcasted_iota(jnp.int32, tri.shape, 0)
    col = lax.broadcasted_iota(jnp.int32, tri.shape, 1)
    tri[...] = jnp.where((col > row) | (row >= positions), 1.0, 0.0).astype(BF16)
    row = lax.broadcasted_iota(jnp.int32, tri_t.shape, 0)
    col = lax.broadcasted_iota(jnp.int32, tri_t.shape, 1)
    tri_t[...] = jnp.where(row > col, 1.0, 0.0).astype(BF16)

    fetch[0].wait()
    fetch[1].wait()
    rows_float = tokens[...].astype(F32)
    scaled = (rows_float * gain1[...]).astype(BF16)
    base = 0
    for i, w in enumerate((wq, wk, wv, wo)):
        fetch[2 + i].wait()
        step = min(CHUNK, w.shape[1])
        for c in range(0, w.shape[1], step):
            a_full[:, base + c:base + c + step] = dot(scaled, w[:, c:c + step])
        base += w.shape[1]
    low_at, sq_at = base, base + LANES
    fetch[6].wait()
    a_full[:, low_at:low_at + LANES] = jnp.zeros((seqs, LANES), F32)
    a_full[:, low_at:low_at + rank] = dot(scaled, low[...])
    a_full[:, sq_at:sq_at + LANES] = jnp.broadcast_to(
        jnp.sum(rows_float * rows_float, axis=1, keepdims=True), (seqs, LANES)
    )
    for d in range(min(n, seqs // spd)):
        a_send[d] = a_full[d * spd:(d + 1) * spd, :]
    pl.semaphore_wait(barrier, n + m - 2)
    ax.start()
    a_recv[me] = a_send[me]

    for i in range(7, 11):
        fetch[i].wait()
    spot = me * positions
    head_of = lax.broadcasted_iota(jnp.int32, (heads, chans), 1) // kc
    head_row = lax.broadcasted_iota(jnp.int32, (heads, chans), 0)

    def decays(g, i):
        s = g * spd + i
        length = len_ref[s]
        pre = lax.dot_general(
            lr[s], dw[...], (((0,), (0,)), ((), ())), preferred_element_type=F32
        ) + bias[...]
        gate = log_sigmoid(pre) * (1.0 / 16.0)
        at = spot + lax.broadcasted_iota(jnp.int32, gate.shape, 0)
        gate = jnp.where(at < length, gate, 0.0)
        high = gate.astype(BF16)
        rest = (gate - high.astype(F32)).astype(BF16)
        suffix = dot(tri[...], high) + dot(tri[...], rest)
        weighting = jnp.exp(suffix[:positions])
        key_copy(s).wait()
        key[s] = (key[s].astype(F32) * weighting).astype(BF16)
        at = spot + lax.broadcasted_iota(jnp.int32, (heads, positions), 1)
        extra = jnp.where(at < length, ext[s], 0.0)
        high = extra.astype(BF16)
        rest = (extra - high.astype(F32)).astype(BF16)
        beyond = dot(high, tri_t[...]) + dot(rest, tri_t[...])
        efac[s, 0:heads, :] = jnp.where(at < length, jnp.exp(beyond), 0.0)
        if heads < 8:
            efac[s, heads:8, :] = jnp.zeros((8 - heads, positions), F32)
        whole = jnp.sum(extra, axis=1, keepdims=True)
        spread = jnp.sum(jnp.where(head_of == head_row, whole, 0.0), axis=0, keepdims=True)
        t_send[g, i:i + 1, :] = suffix[positions:positions + 1] + spread

    def guarded(body, g):
        for i in range(spd):
            if n * spd == seqs:
                body(g, i)
            else:
                pl.when(g * spd + i < seqs)(functools.partial(body, g, i))

    @pl.loop(0, n)
    def _(g):
        guarded(decays, g)

        @pl.when(g != me)
        def _():
            tx.to(g).start()

        @pl.when(g == me)
        def _():
            t_recv[me] = t_send[g]

    ax.wait_recv()
    total = a_recv[0]
    for e in range(1, n):
        total = total + a_recv[e]
    inv = lax.rsqrt(total[:, sq_at:sq_at + 1] / model + NORM_EPSILON)

    def rounded(start, size):
        return (inv * total[:, start:start + size]).astype(BF16)

    query = rounded(0, chans).astype(F32) * kc ** (-0.5)
    fresh_key = rounded(chans, chans).astype(F32)
    fresh_value = rounded(2 * chans, vals).astype(F32)
    outgate = rounded(2 * chans + vals, vals).astype(F32)
    fresh_gate = log_sigmoid(dot(rounded(low_at, rank), dw[...]) + bias[...]) * (1.0 / 16.0)
    qk = query * fresh_key
    tx.wait_recv()
    beyond = fresh_gate
    for e in range(n - 1, -1, -1):
        q_send[e] = query * jnp.exp(beyond)
        beyond = beyond + t_recv[e]
    qx.start()
    q_recv[me] = q_send[me]

    q_head = lax.broadcasted_iota(jnp.int32, (8, chans), 1) // kc
    q_row = lax.broadcasted_iota(jnp.int32, (8, chans), 0)
    v_head = lax.broadcasted_iota(jnp.int32, (8, vals), 1) // dv
    v_row = lax.broadcasted_iota(jnp.int32, (8, vals), 0)

    def mix(g, i):
        s = g * spd + i
        queries = jnp.where(q_head == q_row, q_recv[g, i:i + 1, :], 0.0).astype(BF16)
        scores = lax.dot_general(
            queries, key[s], (((1,), (1,)), ((), ())), preferred_element_type=F32
        ) * efac[s]
        val_copy(s).wait()
        sums = dot(scores.astype(BF16), val[s])
        p_send[g, i:i + 1, :] = jnp.sum(jnp.where(v_head == v_row, sums, 0.0), axis=0, keepdims=True)

    @pl.loop(0, n)
    def _(g):
        @pl.when(g != me)
        def _():
            qx.arrived(g)

        guarded(mix, g)

        @pl.when(g != me)
        def _():
            px.to(g).start()

        @pl.when(g == me)
        def _():
            p_recv[me] = p_send[g]

    fetch[11].wait()
    px.wait_recv()
    mixed = p_recv[0]
    for e in range(1, n):
        mixed = mixed + p_recv[e]
    for h in range(heads):
        own = jnp.sum(qk[:, h * kc:(h + 1) * kc], axis=1, keepdims=True)
        part = slice(h * dv, (h + 1) * dv)
        x = mixed[:, part] + own * fresh_value[:, part]
        mean_sq = jnp.mean(x * x, axis=1, keepdims=True)
        v = outgate[:, part]
        gated = x * lax.rsqrt(mean_sq + NORM_EPSILON) * hgain[...] * (v / (1.0 + jnp.exp(-v)))
        g_own[:, part] = gated
    gx.start()
    g_recv[me] = g_own[...]
    fetch[12].wait()
    gx.wait_recv()
    for d in range(min(n, seqs // spd)):
        g_full[d * spd:(d + 1) * spd, :] = g_recv[d]
    o_own[...] = dot(g_full[...].astype(BF16), wout[...]).astype(BF16)
    ox.start()
    o_recv[mt] = o_own[...]
    fetch[13].wait()
    fetch[14].wait()
    ox.wait_recv()
    attn = o_recv[0].astype(F32)
    for e in range(1, m):
        attn = attn + o_recv[e].astype(F32)
    residual = rows_float + attn

    s_own[...] = jnp.broadcast_to(jnp.sum(residual * residual, axis=1, keepdims=True), s_own.shape)
    sx.start()
    s_recv[me] = s_own[...]
    scaled_two = (residual * gain2[...]).astype(BF16)
    fetch[15].wait()
    for d in range(pl.cdiv(hidden, hw)):
        lo, size = d * hw, min(hw, hidden - d * hw)
        e_send[d, 0:seqs, 0:size] = dot(scaled_two, wg[:, lo:lo + size]).astype(BF16)
        e_send[d, seqs:2 * seqs, 0:size] = dot(scaled_two, wu[:, lo:lo + size]).astype(BF16)
    ex.start()
    e_recv[me] = e_send[me]
    sx.wait_recv()
    sq = s_recv[0]
    for e in range(1, n):
        sq = sq + s_recv[e]
    inv_two = lax.rsqrt(sq[:, 0:1] / model + NORM_EPSILON)
    fetch[16].wait()
    ex.wait_recv()
    both = e_recv[0].astype(F32)
    for e in range(1, n):
        both = both + e_recv[e].astype(F32)
    gate = inv_two * both[0:seqs]
    up = inv_two * both[seqs:2 * seqs]
    h_own[...] = (gate / (1.0 + jnp.exp(-gate)) * up).astype(BF16)
    hx.start()
    h_recv[me] = h_own[...]
    hx.wait_recv()
    down = jnp.zeros((seqs, width), F32)
    for d in range(pl.cdiv(hidden, hw)):
        lo, size = d * hw, min(hw, hidden - d * hw)
        down = down + dot(h_recv[d, :, 0:size], wd[lo:lo + size, :])
    f_own[...] = down.astype(BF16)
    fx.start()
    f_recv[mt] = f_own[...]
    for x in (ax, tx, qx, px, gx, sx, ex, hx, ox):
        x.wait_send()
    fx.wait_recv()
    result = residual
    for e in range(m):
        result = result + f_recv[e].astype(F32)
    out_ref[...] = result.astype(BF16)
    fx.wait_send()


def solution(mesh):
    n, m = mesh.shape["kv"], mesh.shape["tp"]

    def shards(
        tokens, attention_norm_gain, query_weight, key_weight, value_weight, output_gate_weight,
        lowrank_weight, decay_weight, decay_preact_bias, head_norm_gain, output_weight,
        feedforward_norm_gain, feedforward_gate_weight, feedforward_up_weight,
        feedforward_down_weight, past_key_cache, past_value_cache, past_lowrank_cache,
        head_extra_decay, lengths,
    ):
        seqs, width = tokens.shape
        chans, vals = query_weight.shape[1], value_weight.shape[1]
        positions = past_key_cache.shape[1]
        rank = lowrank_weight.shape[1]
        hidden = feedforward_gate_weight.shape[1]
        spd = pl.cdiv(seqs, n)
        hw = pl.cdiv(pl.cdiv(hidden, LANES), n) * LANES
        acols = 2 * chans + 2 * vals + 2 * LANES
        V = pltpu.VMEM

        def like(a):
            return V(a.shape, a.dtype)

        args = (
            tokens, attention_norm_gain[None], query_weight, key_weight, value_weight,
            output_gate_weight, lowrank_weight, decay_weight, decay_preact_bias[None],
            head_norm_gain[None], output_weight, feedforward_norm_gain[None],
            feedforward_gate_weight, feedforward_up_weight, feedforward_down_weight,
            past_key_cache, past_value_cache, past_lowrank_cache, head_extra_decay, lengths,
        )
        scratch = [
            like(tokens), V((1, width), F32), like(query_weight), like(key_weight),
            like(value_weight), like(output_gate_weight), V((width, rank), BF16),
            V((rank, chans), BF16), V((1, chans), F32), V((1, head_norm_gain.shape[0]), F32),
            like(output_weight), V((1, width), F32), like(feedforward_gate_weight),
            like(feedforward_up_weight), like(feedforward_down_weight), like(past_key_cache),
            like(past_value_cache), like(past_lowrank_cache), like(head_extra_decay),
            V((positions + 16, positions), BF16), V((positions, positions), BF16),
            V((seqs, 8, positions), F32), V((seqs, acols), F32),
            V((n, spd, acols), F32), V((n, spd, acols), F32),
            V((n, spd, chans), F32), V((n, spd, chans), F32),
            V((n, spd, chans), F32), V((n, spd, chans), F32),
            V((n, spd, vals), F32), V((n, spd, vals), F32),
            V((spd, vals), F32), V((n, spd, vals), F32), V((seqs, vals), F32),
            V((seqs, width), BF16), V((m, seqs, width), BF16),
            V((seqs, LANES), F32), V((n, seqs, LANES), F32),
            V((n, 2 * seqs, hw), BF16), V((n, 2 * seqs, hw), BF16),
            V((seqs, hw), BF16), V((n, seqs, hw), BF16),
            V((seqs, width), BF16), V((m, seqs, width), BF16),
            pltpu.SemaphoreType.DMA((17,)), pltpu.SemaphoreType.DMA((seqs,)),
            pltpu.SemaphoreType.DMA((seqs,)),
            pltpu.SemaphoreType.DMA((8, n)), pltpu.SemaphoreType.DMA((8, n)),
            pltpu.SemaphoreType.DMA((2, m)), pltpu.SemaphoreType.DMA((2, m)),
        ]
        specs = [pl.BlockSpec(memory_space=pl.ANY)] * (len(args) - 1)
        specs.append(pl.BlockSpec(memory_space=pltpu.SMEM))
        return pl.pallas_call(
            functools.partial(layer, n, m, spd),
            out_shape=jax.ShapeDtypeStruct((seqs, width), BF16),
            in_specs=specs,
            out_specs=pl.BlockSpec(memory_space=V),
            scratch_shapes=scratch,
            compiler_params=pltpu.CompilerParams(
                collective_id=0, has_side_effects=True, vmem_limit_bytes=64_000_000
            ),
        )(*args)

    return jax.shard_map(
        shards,
        mesh=mesh,
        in_specs=(
            P(None, "kv"), P(), P("kv", "tp"), P("kv", "tp"), P("kv", "tp"), P("kv", "tp"),
            P(), P(), P(), P(), P("tp", "kv"), P(), P("kv", "tp"), P("kv", "tp"),
            P("tp", "kv"), P(None, "kv", "tp"), P(None, "kv", "tp"), P(None, None, "kv"),
            P(None, "tp", "kv"), P(),
        ),
        out_specs=P(None, "kv"),
        check_vma=False,
    )
```

```python
import functools

import jax
import jax.numpy as jnp
from jax import lax
from jax.experimental import pallas as pl
from jax.experimental.pallas import tpu as pltpu
from jax.sharding import PartitionSpec as P

NORM_EPSILON = 1e-06
LANES = 128
CHUNK = 512
F32 = jnp.float32
BF16 = jnp.bfloat16


def dot(a, b):
    return jnp.dot(a, b, preferred_element_type=F32)


def log_sigmoid(v):
    return jnp.minimum(v, 0.0) - jnp.log(1.0 + jnp.exp(-jnp.abs(v)))


def remote(src, dst, send_sem, recv_sem, axis, dest):
    return pltpu.make_async_remote_copy(
        src_ref=src,
        dst_ref=dst,
        send_sem=send_sem,
        recv_sem=recv_sem,
        device_id={axis: dest},
        device_id_type=pl.DeviceIdType.MESH,
    )


class Exchange:
    def __init__(self, axis, size, out, slots, send_sem, recv_sem, same=False):
        self.axis, self.size, self.out, self.slots = axis, size, out, slots
        self.send_sem, self.recv_sem, self.same = send_sem, recv_sem, same
        self.me = lax.axis_index(axis)

    def source(self, dest):
        return self.out if self.same else self.out.at[dest]

    def to(self, dest):
        return remote(
            self.source(dest), self.slots.at[self.me], self.send_sem.at[dest],
            self.recv_sem.at[self.me], self.axis, dest,
        )

    def start(self):
        for k in range(1, self.size):
            self.to(lax.rem(self.me + k, self.size)).start()

    def arrived(self, origin):
        remote(
            self.source(origin), self.slots.at[origin], self.send_sem.at[origin],
            self.recv_sem.at[origin], self.axis, origin,
        ).wait_recv()

    def wait_recv(self):
        for k in range(1, self.size):
            self.arrived(lax.rem(self.me + k, self.size))

    def wait_send(self):
        for k in range(1, self.size):
            self.to(lax.rem(self.me + k, self.size)).wait_send()


def layer(
    n, m, spd,
    tokens_h, gain1_h, wq_h, wk_h, wv_h, wo_h, low_h, dw_h, bias_h, hgain_h, wout_h,
    gain2_h, wg_h, wu_h, wd_h, key_h, val_h, lr_h, ext_h, len_ref,
    out_ref,
    tokens, gain1, wq, wk, wv, wo, low, dw, bias, hgain, wout, gain2, wg, wu, wd,
    key, val, lr, ext,
    tri, tri_t, efac, a_full, a_send, a_recv, t_send, t_recv, q_send, q_recv,
    p_send, p_recv, g_own, g_recv, g_full, o_own, o_recv, s_own, s_recv,
    u_send, u_recv, e_send, e_recv, h_own, h_recv, f_own, f_recv,
    in_sem, key_sem, val_sem, kv_ss, kv_rs, tp_ss, tp_rs, u_ss, u_rs,
):
    me = lax.axis_index("kv")
    mt = lax.axis_index("tp")
    seqs, width = tokens.shape
    chans, vals = wq.shape[1], wv.shape[1]
    heads, positions = ext.shape[1], ext.shape[2]
    kc, dv = chans // heads, vals // heads
    rank = low.shape[0]
    hidden = wg.shape[1]
    hw = e_send.shape[2]
    model = width * n

    def cols_of(ref, start, size):
        return ref.at[:, pl.ds(pl.multiple_of(start, size), size)]

    sources = [
        (tokens_h, tokens),
        (cols_of(gain1_h, me * width, width), gain1),
        (wq_h, wq), (wk_h, wk), (wv_h, wv), (wo_h, wo),
        (cols_of(low_h, me * width, width), low),
        (cols_of(dw_h, mt * chans, chans), dw),
        (cols_of(bias_h, mt * chans, chans), bias),
        (lr_h, lr), (ext_h, ext),
    ]
    later = [
        (hgain_h, hgain), (wout_h, wout),
        (cols_of(gain2_h, me * width, width), gain2),
        (wg_h, wg), (wu_h, wu), (wd_h, wd),
    ]
    fetch = [pltpu.make_async_copy(a, b, in_sem.at[i]) for i, (a, b) in enumerate(sources + later)]
    for c in fetch[:len(sources)]:
        c.start()

    def key_copy(s):
        return pltpu.make_async_copy(key_h.at[s], key.at[s], key_sem.at[s])

    def val_copy(s):
        return pltpu.make_async_copy(val_h.at[s], val.at[s], val_sem.at[s])

    pl.loop(0, seqs)(lambda s: key_copy(s).start())
    pl.loop(0, seqs)(lambda s: val_copy(s).start())
    for c in fetch[len(sources):]:
        c.start()

    barrier = pltpu.get_barrier_semaphore()
    for axis, size, own in (("kv", n, me), ("tp", m, mt)):
        for k in range(1, size):
            pl.semaphore_signal(
                barrier, inc=1, device_id={axis: lax.rem(own + k, size)},
                device_id_type=pl.DeviceIdType.MESH,
            )

    def kv_exchange(i, out, slots, same=False):
        return Exchange("kv", n, out, slots, kv_ss.at[i], kv_rs.at[i], same)

    def tp_exchange(i, out, slots):
        return Exchange("tp", m, out, slots, tp_ss.at[i], tp_rs.at[i], True)

    ax = kv_exchange(0, a_send, a_recv)
    tx = kv_exchange(1, t_send, t_recv)
    qx = kv_exchange(2, q_send, q_recv)
    px = kv_exchange(3, p_send, p_recv)
    gx = kv_exchange(4, g_own, g_recv, True)
    sx = kv_exchange(5, s_own, s_recv, True)
    zs = n // 2
    z, core = lax.div(me, 2), lax.rem(me, 2)
    partner = me + 1 - 2 * core

    def u_copy(zc):
        return remote(u_send.at[2 * zc + 1 - core], u_recv.at[zc], u_ss.at[zc], u_rs.at[zc], "kv", partner)

    def e_copy(zc, slot):
        return remote(
            e_send.at[zc], e_recv.at[slot], kv_ss.at[6, zc], kv_rs.at[6, slot], "kv", 2 * zc + core
        )

    def h_copy(src, slot, send, dest):
        return remote(src, h_recv.at[slot], kv_ss.at[7, send], kv_rs.at[7, slot], "kv", dest)

    ox = tp_exchange(0, o_own, o_recv)
    fx = tp_exchange(1, f_own, f_recv)

    row = lax.broadcasted_iota(jnp.int32, tri.shape, 0)
    col = lax.broadcasted_iota(jnp.int32, tri.shape, 1)
    tri[...] = jnp.where((col > row) | (row >= positions), 1.0, 0.0).astype(BF16)
    row = lax.broadcasted_iota(jnp.int32, tri_t.shape, 0)
    col = lax.broadcasted_iota(jnp.int32, tri_t.shape, 1)
    tri_t[...] = jnp.where(row > col, 1.0, 0.0).astype(BF16)

    fetch[0].wait()
    fetch[1].wait()
    rows_float = tokens[...].astype(F32)
    scaled = (rows_float * gain1[...]).astype(BF16)
    base = 0
    for i, w in enumerate((wq, wk, wv, wo)):
        fetch[2 + i].wait()
        step = min(CHUNK, w.shape[1])
        for c in range(0, w.shape[1], step):
            a_full[:, base + c:base + c + step] = dot(scaled, w[:, c:c + step])
        base += w.shape[1]
    low_at, sq_at = base, base + LANES
    fetch[6].wait()
    a_full[:, low_at:low_at + LANES] = jnp.zeros((seqs, LANES), F32)
    a_full[:, low_at:low_at + rank] = lax.dot_general(
        scaled, low[...], (((1,), (1,)), ((), ())), preferred_element_type=F32
    )
    a_full[:, sq_at:sq_at + LANES] = jnp.broadcast_to(
        jnp.sum(rows_float * rows_float, axis=1, keepdims=True), (seqs, LANES)
    )
    for d in range(min(n, seqs // spd)):
        a_send[d] = a_full[d * spd:(d + 1) * spd, :].astype(BF16)
    pl.semaphore_wait(barrier, n + m - 2)
    ax.start()
    a_recv[me] = a_send[me]

    for i in range(7, 11):
        fetch[i].wait()
    spot = me * positions
    head_of = lax.broadcasted_iota(jnp.int32, (heads, chans), 1) // kc
    head_row = lax.broadcasted_iota(jnp.int32, (heads, chans), 0)

    def decays(g, i):
        s = g * spd + i
        length = len_ref[s]
        pre = lax.dot_general(
            lr[s], dw[...], (((0,), (0,)), ((), ())), preferred_element_type=F32
        ) + bias[...]
        gate = log_sigmoid(pre) * (1.0 / 16.0)
        at = spot + lax.broadcasted_iota(jnp.int32, gate.shape, 0)
        gate = jnp.where(at < length, gate, 0.0)
        high = gate.astype(BF16)
        rest = (gate - high.astype(F32)).astype(BF16)
        suffix = dot(tri[...], high) + dot(tri[...], rest)
        weighting = jnp.exp(suffix[:positions])
        key_copy(s).wait()
        key[s] = (key[s].astype(F32) * weighting).astype(BF16)
        at = spot + lax.broadcasted_iota(jnp.int32, (heads, positions), 1)
        extra = jnp.where(at < length, ext[s], 0.0)
        high = extra.astype(BF16)
        rest = (extra - high.astype(F32)).astype(BF16)
        beyond = dot(high, tri_t[...]) + dot(rest, tri_t[...])
        efac[s, 0:heads, :] = jnp.where(at < length, jnp.exp(beyond), 0.0)
        if heads < 8:
            efac[s, heads:8, :] = jnp.zeros((8 - heads, positions), F32)
        whole = jnp.sum(extra, axis=1, keepdims=True)
        spread = jnp.sum(jnp.where(head_of == head_row, whole, 0.0), axis=0, keepdims=True)
        t_send[g, i:i + 1, :] = suffix[positions:positions + 1] + spread

    def guarded(body, g):
        for i in range(spd):
            if n * spd == seqs:
                body(g, i)
            else:
                pl.when(g * spd + i < seqs)(functools.partial(body, g, i))

    @pl.loop(0, n)
    def _(g):
        guarded(decays, g)

        @pl.when(g != me)
        def _():
            tx.to(g).start()

        @pl.when(g == me)
        def _():
            t_recv[me] = t_send[g]

    ax.wait_recv()
    total = a_recv[0].astype(F32)
    for e in range(1, n):
        total = total + a_recv[e].astype(F32)
    inv = lax.rsqrt(total[:, sq_at:sq_at + 1] / model + NORM_EPSILON)

    def rounded(start, size):
        return (inv * total[:, start:start + size]).astype(BF16)

    query = rounded(0, chans).astype(F32) * kc ** (-0.5)
    fresh_key = rounded(chans, chans).astype(F32)
    fresh_value = rounded(2 * chans, vals).astype(F32)
    outgate = rounded(2 * chans + vals, vals).astype(F32)
    fresh_gate = log_sigmoid(dot(rounded(low_at, rank), dw[...]) + bias[...]) * (1.0 / 16.0)
    qk = query * fresh_key
    tx.wait_recv()
    beyond = fresh_gate
    for e in range(n - 1, -1, -1):
        q_send[e] = query * jnp.exp(beyond)
        beyond = beyond + t_recv[e]
    qx.start()
    q_recv[me] = q_send[me]

    q_head = lax.broadcasted_iota(jnp.int32, (8, chans), 1) // kc
    q_row = lax.broadcasted_iota(jnp.int32, (8, chans), 0)
    v_head = lax.broadcasted_iota(jnp.int32, (8, vals), 1) // dv
    v_row = lax.broadcasted_iota(jnp.int32, (8, vals), 0)

    def mix(g, i):
        s = g * spd + i
        queries = jnp.where(q_head == q_row, q_recv[g, i:i + 1, :], 0.0).astype(BF16)
        scores = lax.dot_general(
            queries, key[s], (((1,), (1,)), ((), ())), preferred_element_type=F32
        ) * efac[s]
        val_copy(s).wait()
        sums = dot(scores.astype(BF16), val[s])
        p_send[g, i:i + 1, :] = jnp.sum(jnp.where(v_head == v_row, sums, 0.0), axis=0, keepdims=True)

    @pl.loop(0, n)
    def _(g):
        @pl.when(g != me)
        def _():
            qx.arrived(g)

        guarded(mix, g)

        @pl.when(g != me)
        def _():
            px.to(g).start()

        @pl.when(g == me)
        def _():
            p_recv[me] = p_send[g]

    fetch[11].wait()
    px.wait_recv()
    mixed = p_recv[0]
    for e in range(1, n):
        mixed = mixed + p_recv[e]
    for h in range(heads):
        own = jnp.sum(qk[:, h * kc:(h + 1) * kc], axis=1, keepdims=True)
        part = slice(h * dv, (h + 1) * dv)
        x = mixed[:, part] + own * fresh_value[:, part]
        mean_sq = jnp.mean(x * x, axis=1, keepdims=True)
        v = outgate[:, part]
        gated = x * lax.rsqrt(mean_sq + NORM_EPSILON) * hgain[...] * (v / (1.0 + jnp.exp(-v)))
        g_own[:, part] = gated.astype(BF16)
    gx.start()
    g_recv[me] = g_own[...]
    fetch[12].wait()
    gx.wait_recv()
    for d in range(min(n, seqs // spd)):
        g_full[d * spd:(d + 1) * spd, :] = g_recv[d].astype(F32)
    o_own[...] = dot(g_full[...].astype(BF16), wout[...]).astype(BF16)
    ox.start()
    o_recv[mt] = o_own[...]
    fetch[13].wait()
    fetch[14].wait()
    ox.wait_recv()
    attn = o_recv[0].astype(F32)
    for e in range(1, m):
        attn = attn + o_recv[e].astype(F32)
    residual = rows_float + attn

    s_own[...] = jnp.broadcast_to(jnp.sum(residual * residual, axis=1, keepdims=True), s_own.shape)
    sx.start()
    s_recv[me] = s_own[...]
    scaled_two = (residual * gain2[...]).astype(BF16)
    fetch[15].wait()
    for d in range(n):
        lo, size = d * hw, min(hw, hidden - d * hw)
        if size > 0:
            u_send[d, 0:seqs, 0:size] = dot(scaled_two, wg[:, lo:lo + size]).astype(BF16)
            u_send[d, seqs:2 * seqs, 0:size] = dot(scaled_two, wu[:, lo:lo + size]).astype(BF16)
        if d % 2:
            u_copy(d // 2).start()
    for k in range(1, zs + 1):
        zc = lax.rem(z + k, zs)
        u_copy(zc).wait_recv()
        pair = u_send[2 * zc + core].astype(F32) + u_recv[zc].astype(F32)
        if k < zs:
            e_send[zc] = pair.astype(BF16)
            e_copy(zc, z).start()
        else:
            e_recv[z] = pair.astype(BF16)
    sx.wait_recv()
    sq = s_recv[0]
    for e in range(1, n):
        sq = sq + s_recv[e]
    inv_two = lax.rsqrt(sq[:, 0:1] / model + NORM_EPSILON)
    fetch[16].wait()
    for k in range(1, zs):
        zc = lax.rem(z + k, zs)
        e_copy(zc, zc).wait_recv()
    both = e_recv[0].astype(F32)
    for e in range(1, zs):
        both = both + e_recv[e].astype(F32)
    gate = inv_two * both[0:seqs]
    up = inv_two * both[seqs:2 * seqs]
    h_own[...] = (gate / (1.0 + jnp.exp(-gate)) * up).astype(BF16)
    for k in range(1, zs):
        dest = 2 * lax.rem(z + k, zs) + core
        h_copy(h_own, me, dest, dest).start()
    h_copy(h_own, me, partner, partner).start()
    h_recv[me] = h_own[...]
    for k in range(1, zs):
        zc = lax.rem(z + k, zs)
        origin = 2 * zc + core
        h_copy(h_own, origin, origin, origin).wait_recv()
        h_copy(h_recv.at[origin], origin, 2 * zc + 1 - core, partner).start()
    for k in range(zs):
        origin = 2 * lax.rem(z + k, zs) + 1 - core
        h_copy(h_own, origin, origin, partner).wait_recv()
    down = jnp.zeros((seqs, width), F32)
    for d in range(pl.cdiv(hidden, hw)):
        lo, size = d * hw, min(hw, hidden - d * hw)
        down = down + dot(h_recv[d, :, 0:size], wd[lo:lo + size, :])
    f_own[...] = down.astype(BF16)
    fx.start()
    f_recv[mt] = f_own[...]
    for x in (ax, tx, qx, px, gx, sx, ox):
        x.wait_send()
    for k in range(zs):
        zc = lax.rem(z + k, zs)
        u_copy(zc).wait_send()
        h_copy(h_own, me, 2 * zc + 1 - core, partner).wait_send()
        if k > 0:
            e_copy(zc, z).wait_send()
            h_copy(h_own, me, 2 * zc + core, partner).wait_send()
    fx.wait_recv()
    result = residual
    for e in range(m):
        result = result + f_recv[e].astype(F32)
    out_ref[...] = result.astype(BF16)
    fx.wait_send()


def solution(mesh):
    n, m = mesh.shape["kv"], mesh.shape["tp"]

    def shards(
        tokens, attention_norm_gain, query_weight, key_weight, value_weight, output_gate_weight,
        lowrank_weight, decay_weight, decay_preact_bias, head_norm_gain, output_weight,
        feedforward_norm_gain, feedforward_gate_weight, feedforward_up_weight,
        feedforward_down_weight, past_key_cache, past_value_cache, past_lowrank_cache,
        head_extra_decay, lengths,
    ):
        seqs, width = tokens.shape
        chans, vals = query_weight.shape[1], value_weight.shape[1]
        positions = past_key_cache.shape[1]
        rank = lowrank_weight.shape[1]
        hidden = feedforward_gate_weight.shape[1]
        spd = pl.cdiv(seqs, n)
        hw = pl.cdiv(pl.cdiv(hidden, LANES), n) * LANES
        acols = 2 * chans + 2 * vals + 2 * LANES
        V = pltpu.VMEM

        def like(a):
            return V(a.shape, a.dtype)

        args = (
            tokens, attention_norm_gain[None], query_weight, key_weight, value_weight,
            output_gate_weight, lowrank_weight.T, decay_weight, decay_preact_bias[None],
            head_norm_gain[None], output_weight, feedforward_norm_gain[None],
            feedforward_gate_weight, feedforward_up_weight, feedforward_down_weight,
            past_key_cache, past_value_cache, past_lowrank_cache, head_extra_decay, lengths,
        )
        scratch = [
            like(tokens), V((1, width), F32), like(query_weight), like(key_weight),
            like(value_weight), like(output_gate_weight), V((rank, width), BF16),
            V((rank, chans), BF16), V((1, chans), F32), V((1, head_norm_gain.shape[0]), F32),
            like(output_weight), V((1, width), F32), like(feedforward_gate_weight),
            like(feedforward_up_weight), like(feedforward_down_weight), like(past_key_cache),
            like(past_value_cache), like(past_lowrank_cache), like(head_extra_decay),
            V((positions + 16, positions), BF16), V((positions, positions), BF16),
            V((seqs, 8, positions), F32), V((seqs, acols), F32),
            V((n, spd, acols), BF16), V((n, spd, acols), BF16),
            V((n, spd, chans), F32), V((n, spd, chans), F32),
            V((n, spd, chans), F32), V((n, spd, chans), F32),
            V((n, spd, vals), F32), V((n, spd, vals), F32),
            V((spd, vals), BF16), V((n, spd, vals), BF16), V((seqs, vals), F32),
            V((seqs, width), BF16), V((m, seqs, width), BF16),
            V((seqs, LANES), F32), V((n, seqs, LANES), F32),
            V((n, 2 * seqs, hw), BF16), V((n // 2, 2 * seqs, hw), BF16),
            V((n // 2, 2 * seqs, hw), BF16), V((n // 2, 2 * seqs, hw), BF16),
            V((seqs, hw), BF16), V((n, seqs, hw), BF16),
            V((seqs, width), BF16), V((m, seqs, width), BF16),
            pltpu.SemaphoreType.DMA((17,)), pltpu.SemaphoreType.DMA((seqs,)),
            pltpu.SemaphoreType.DMA((seqs,)),
            pltpu.SemaphoreType.DMA((8, n)), pltpu.SemaphoreType.DMA((8, n)),
            pltpu.SemaphoreType.DMA((2, m)), pltpu.SemaphoreType.DMA((2, m)),
            pltpu.SemaphoreType.DMA((n // 2,)), pltpu.SemaphoreType.DMA((n // 2,)),
        ]
        specs = [pl.BlockSpec(memory_space=pl.ANY)] * (len(args) - 1)
        specs.append(pl.BlockSpec(memory_space=pltpu.SMEM))
        return pl.pallas_call(
            functools.partial(layer, n, m, spd),
            out_shape=jax.ShapeDtypeStruct((seqs, width), BF16),
            in_specs=specs,
            out_specs=pl.BlockSpec(memory_space=V),
            scratch_shapes=scratch,
            compiler_params=pltpu.CompilerParams(
                collective_id=0, has_side_effects=True, vmem_limit_bytes=64_000_000
            ),
        )(*args)

    return jax.shard_map(
        shards,
        mesh=mesh,
        in_specs=(
            P(None, "kv"), P(), P("kv", "tp"), P("kv", "tp"), P("kv", "tp"), P("kv", "tp"),
            P(), P(), P(), P(), P("tp", "kv"), P(), P("kv", "tp"), P("kv", "tp"),
            P("tp", "kv"), P(None, "kv", "tp"), P(None, "kv", "tp"), P(None, None, "kv"),
            P(None, "tp", "kv"), P(),
        ),
        out_specs=P(None, "kv"),
        check_vma=False,
    )
```
